32 devices in a mesh: grp: 2 (over x), ep: 16 (over z, y, core).
Axes of the slice: x: 2, y: 2, z: 4, core: 2. Of those that a mesh axis runs over, the one named last changes fastest.
Arguments:
- tokens: bfloat16 [256, 2048], P(('grp', 'ep')), parts along dimension 0, may hold values from -6 to 6
- first_gain: bfloat16 [2048], replicated, may hold values from 0.099609375 to 1.8984375
- query_weight: bfloat16 [2048, 1024], P(None, 'ep'), may hold values from -0.125 to 0.125
- key_weight: bfloat16 [2048, 1024], P(None, 'ep'), may hold values from -0.125 to 0.125
- value_weight: bfloat16 [2048, 1024], P(None, 'ep'), may hold values from -0.125 to 0.125
- outgate_weight: bfloat16 [2048, 1024], P(None, 'ep'), may hold values from -0.125 to 0.125
- igate_weight: bfloat16 [2048, 8], replicated, may hold values from -0.125 to 0.125
- fgate_weight: bfloat16 [2048, 8], replicated, may hold values from -0.125 to 0.125
- igate_bias: float32 [8], replicated, may hold values from -2 to 1
- fgate_bias: float32 [8], replicated, may hold values from -1 to 4
- memory_state: float32 [256, 8, 128, 128], P(('grp', 'ep')), parts along dimension 0, may hold values from -0.6 to 0.6
- norm_state: float32 [256, 8, 128], P(('grp', 'ep')), parts along dimension 0, may hold values from -0.6 to 0.6
- max_state: float32 [256, 8], P(('grp', 'ep')), parts along dimension 0, may hold values from -1 to 2
- head_gain: bfloat16 [1024], replicated, may hold values from 0.099609375 to 1.8984375
- out_weight: bfloat16 [1024, 2048], P('ep'), may hold values from -0.1875 to 0.1875
- second_gain: bfloat16 [2048], replicated, may hold values from 0.099609375 to 1.8984375
- expert_ids: int32 [256, 6], P(('grp', 'ep')), parts along dimension 0, may hold values from 0 to 15, all different within a row; in each aligned block of 8 rows (0 to 7, 8 to 15, ...) at most 6 rows name the same one
- route_weight: float32 [256, 6], P(('grp', 'ep')), parts along dimension 0, may hold values from 0.2 to 1
- expert_gate: bfloat16 [16, 2048, 256], P('ep'), may hold values from -0.125 to 0.125
- expert_up: bfloat16 [16, 2048, 256], P('ep'), may hold values from -0.125 to 0.125
- expert_down: bfloat16 [16, 256, 2048], P('ep'), may hold values from -0.375 to 0.375
- shared_gate: bfloat16 [2048, 256], P('ep'), may hold values from -0.125 to 0.125
- shared_up: bfloat16 [2048, 256], P('ep'), may hold values from -0.125 to 0.125
- shared_down: bfloat16 [256, 2048], P(None, 'ep'), may hold values from -0.375 to 0.375
Outputs:
- mixed_out: bfloat16 [256, 2048], P(('grp', 'ep')), parts along dimension 0
- memory_next: float32 [256, 8, 128, 128], P(('grp', 'ep')), parts along dimension 0
- norm_next: float32 [256, 8, 128], P(('grp', 'ep')), parts along dimension 0
- max_next: float32 [256, 8], P(('grp', 'ep')), parts along dimension 0
The draws below stay inside these ranges and needn't reach their ends.
There are 2 independent parts, one for each index of `grp`. The reference program is written for one: setup_inputs(seed, part) draws one part's arguments, and reference() takes and returns one part's arrays. A program takes and returns all parts, laid end to end along the dimension named above; an argument that names none is the same for every part. Nothing has to cross between parts.
Inputs may be any that keep to these rules, and one draw needn't show every extreme that they name: `expert_ids`: each row names 6 different experts. Among the rows of one device no expert is named by more than 6 rows, and in every draw some expert is named by exactly 6 rows of some device.
All inputs are finite; a program needn't handle non-finite values.
Results may differ from the reference program's by a relative error of at most 0.013.
Values may be sent and summed in bfloat16 or wider, within the bound.
No kernel may reach another device: no remote copies, remote signals or barrier semaphores. Data moves between devices by JAX's collectives and lax.ppermute only.
A program may use at most 64 MiB of HBM per device.

```python
import math
import jax
import jax.numpy as jnp
import numpy as np
from jax import lax

D = 2048
HEADS = 8
DK = 128
FE = 256
FS = 256
TOP_K = 6
SEQ_DEV = 8
MW = 1024
SEQS = 128
EXPERTS = 16
CAP = 6
N_EP = 16


def levels(own_key, shape, pieces, low, high):
    loudness, own = 1.0, jax.random.fold_in(own_key, 6)
    for axis_at, parts in pieces:
        draws = jnp.exp(jax.random.uniform(jax.random.fold_in(own, axis_at), (parts,), jnp.float32, low / len(pieces), high / len(pieces)))
        loudness = loudness * jnp.repeat(draws, shape[axis_at] // parts).reshape([-1 if axis == axis_at else 1 for axis in range(len(shape))])
    return loudness


def routed_block(key, own, number, rows, number_of, top, reach, slope):
    sequence = jax.random.permutation(key, number_of)
    crowded, usual = portions_of(number_of, rows * top, reach, slope, True), portions_of(number_of, rows * top, reach, slope, False)
    places = jnp.arange(number_of)

    def named(tallies, turn):
        used = int((tallies > 0).sum())
        fixed = max(1, used // 4)
        shifted = fixed + (places - fixed + turn * (used - fixed)) % max(1, number_of - fixed)
        return jnp.zeros((number_of,), jnp.int32).at[sequence[jnp.where(places < fixed, places, shifted)]].set(jnp.asarray(tallies, jnp.int32))

    tallies = jnp.where(number % 4 == 0, named(crowded, number // 4), named(usual, number - number // 4 - 1))
    mixed = jax.random.permutation(jax.random.fold_in(own, 3), number_of)
    giver, sink = mixed[0:number_of // 2 * 2:2], mixed[1:number_of // 2 * 2:2]
    room = jnp.minimum(tallies[giver] - 1, reach - tallies[sink]) // 2
    room = jnp.where((giver == sequence[0]) | (sink == sequence[0]) | (tallies[sink] == 0), 0, jnp.maximum(room, 0))
    shifted = jax.random.randint(jax.random.fold_in(own, 4), (number_of // 2,), 0, 1 << 20) % (room + 1)
    tallies = tallies.at[giver].add(-shifted).at[sink].add(shifted)
    items = jnp.searchsorted(jnp.cumsum(tallies), jnp.arange(rows * top), side="right").astype(jnp.int32)
    listing = items.reshape(top, rows).T
    listing = listing[jax.random.permutation(jax.random.fold_in(own, 1), rows)]
    turn = jax.random.randint(jax.random.fold_in(own, 2), (rows, 1), 0, top)
    return jnp.take_along_axis(listing, (jnp.arange(top)[None, :] + turn) % top, axis=1)


def portions_of(number_of, total, limit, slope, full):
    portions = [(1 << 20) // math.isqrt(rank ** slope) + 1 for rank in range(1, number_of + 1)]
    largest = limit if full else min(limit, max(-(-total // number_of), total * portions[0] // sum(portions)))
    least = 1 if total - largest >= number_of - 1 else 0
    given, rest = [largest] + [least] * (number_of - 1), total - largest - least * (number_of - 1)
    while rest > 0:
        candidates = [i for i in range(1, number_of) if given[i] < largest] or [i for i in range(1, number_of) if given[i] < limit]
        mass, budget = sum([portions[i] for i in candidates]), rest
        for i in candidates:
            addition = min(limit - given[i], max(1, budget * portions[i] // mass), rest)
            given[i] = given[i] + addition
            rest = rest - addition
    return np.array(given)


def noise(key, shape, spread, limit, split=(), kind=jnp.bfloat16):
    loudness = levels(key, shape, split, -0.22, 0.18) if split else 1.0
    drawn = jax.random.normal(key, shape, jnp.float32) * spread * loudness
    return jnp.minimum(jnp.maximum(drawn, -limit), limit).astype(kind)


def setup_inputs(seed: int = 0, part: int = 0) -> dict:
    arg_keys = jax.random.split(jax.random.key(seed), 25)
    own_keys = jax.random.split(jax.random.fold_in(arg_keys[24], part), 25)
    tokens = noise(own_keys[0], (SEQS, D), 1.0, 6.0, ((0, 16),))
    first_gain = jnp.clip(1.0 + 0.18 * jax.random.normal(arg_keys[1], (D,), jnp.float32), 0.099609375, 1.8984375).astype(jnp.bfloat16)
    query_weight = noise(arg_keys[2], (D, MW), D ** -0.5, 0.125, ((1, 16),))
    key_weight = noise(arg_keys[3], (D, MW), D ** -0.5, 0.125, ((1, 16),))
    value_weight = noise(arg_keys[4], (D, MW), D ** -0.5, 0.125, ((1, 16),))
    outgate_weight = noise(arg_keys[5], (D, MW), D ** -0.5, 0.125, ((1, 16),))
    igate_weight = noise(arg_keys[6], (D, HEADS), D ** -0.5, 0.125)
    fgate_weight = noise(arg_keys[7], (D, HEADS), D ** -0.5, 0.125)
    igate_bias = jnp.clip(jax.random.uniform(arg_keys[8], (HEADS,), jnp.float32, -2.0, 1.0), -2.0, 1.0)
    fgate_bias = jnp.clip(jax.random.uniform(arg_keys[9], (HEADS,), jnp.float32, -1.0, 4.0), -1.0, 4.0)
    memory_state = noise(own_keys[10], (SEQS, HEADS, DK, DK), 0.1, 0.6, ((0, 16),), jnp.float32)
    norm_state = noise(own_keys[11], (SEQS, HEADS, DK), 0.1, 0.6, ((0, 16),), jnp.float32)
    max_state = jnp.clip(-1.0 + 3.0 * jax.random.uniform(own_keys[12], (SEQS, HEADS), jnp.float32) ** levels(own_keys[12], (SEQS, HEADS), ((0, 16),), -0.2, 0.2), -1.0, 2.0)
    head_gain = jnp.clip(1.0 + 0.18 * jax.random.normal(arg_keys[13], (MW,), jnp.float32), 0.099609375, 1.8984375).astype(jnp.bfloat16)
    out_weight = noise(arg_keys[14], (MW, D), MW ** -0.5, 0.1875, ((0, 16),))
    second_gain = jnp.clip(1.0 + 0.18 * jax.random.normal(arg_keys[15], (D,), jnp.float32), 0.099609375, 1.8984375).astype(jnp.bfloat16)
    expert_ids_keys = jax.random.split(jax.random.fold_in(own_keys[16], 1), SEQS // SEQ_DEV)
    expert_ids_turns = jax.random.permutation(jax.random.fold_in(own_keys[16], 3), SEQS // SEQ_DEV)
    expert_ids = jax.vmap(lambda own, number: routed_block(jax.random.fold_in(own_keys[16], 2), own, number, SEQ_DEV, EXPERTS, TOP_K, CAP, 1))(expert_ids_keys, expert_ids_turns).reshape((SEQS, TOP_K))
    route_weight = jnp.clip(0.2 + 0.8 * jax.random.uniform(own_keys[17], (SEQS, TOP_K), jnp.float32) ** levels(own_keys[17], (SEQS, TOP_K), ((0, 16),), -0.2, 0.2), 0.2, 1.0)
    expert_gate = noise(arg_keys[18], (EXPERTS, D, FE), D ** -0.5, 0.125, ((0, 16),))
    expert_up = noise(arg_keys[19], (EXPERTS, D, FE), D ** -0.5, 0.125, ((0, 16),))
    expert_down = noise(arg_keys[20], (EXPERTS, FE, D), FE ** -0.5, 0.375, ((0, 16),))
    shared_gate = noise(arg_keys[21], (D, FS), D ** -0.5, 0.125, ((0, 16),))
    shared_up = noise(arg_keys[22], (D, FS), D ** -0.5, 0.125, ((0, 16),))
    shared_down = noise(arg_keys[23], (FS, D), FS ** -0.5, 0.375, ((1, 16),))
    return dict(tokens=tokens, first_gain=first_gain, query_weight=query_weight, key_weight=key_weight, value_weight=value_weight, outgate_weight=outgate_weight, igate_weight=igate_weight, fgate_weight=fgate_weight, igate_bias=igate_bias, fgate_bias=fgate_bias, memory_state=memory_state, norm_state=norm_state, max_state=max_state, head_gain=head_gain, out_weight=out_weight, second_gain=second_gain, expert_ids=expert_ids, route_weight=route_weight, expert_gate=expert_gate, expert_up=expert_up, expert_down=expert_down, shared_gate=shared_gate, shared_up=shared_up, shared_down=shared_down)


epsilon = 1e-06

def rms_scale(values, gain):
    return values * lax.rsqrt(lax.optimization_barrier(jnp.mean(values * values, axis=-1, keepdims=True)) + epsilon) * gain.astype(jnp.float32)

def cell_step(normed, query, key_proj, value_proj, outgate, igate_weight, fgate_weight, igate_bias, fgate_bias, memory_state, norm_state, max_state, head_gain):
    row_count, head_count = max_state.shape
    head_size = memory_state.shape[-1]
    input_gate = jnp.dot(normed, igate_weight, preferred_element_type=jnp.float32) + igate_bias
    forget_log = jax.nn.log_sigmoid(jnp.dot(normed, fgate_weight, preferred_element_type=jnp.float32) + fgate_bias)
    query_heads = query.astype(jnp.float32).reshape(row_count, head_count, head_size)
    key_heads = key_proj.astype(jnp.float32).reshape(row_count, head_count, head_size) * head_size ** (-0.5)
    value_heads = value_proj.astype(jnp.float32).reshape(row_count, head_count, head_size)
    max_next = jnp.maximum(forget_log + max_state, input_gate)
    decay_rate = jnp.exp(forget_log + max_state - max_next)
    injected = jnp.exp(input_gate - max_next)
    memory_next = decay_rate[:, :, None, None] * memory_state + injected[:, :, None, None] * (key_heads[:, :, :, None] * value_heads[:, :, None, :])
    norm_next = decay_rate[:, :, None] * norm_state + injected[:, :, None] * key_heads
    numerator = jnp.einsum('shd,shde->she', query_heads, memory_next, precision=lax.Precision.HIGHEST)
    denominator = jnp.maximum(jnp.abs(lax.optimization_barrier(jnp.sum(query_heads * norm_next, axis=-1))), jnp.exp(-max_next))
    readout = numerator / denominator[:, :, None]
    readout = rms_scale(readout, head_gain.reshape(head_count, head_size))
    gated = readout.reshape(row_count, head_count * head_size) * jax.nn.sigmoid(outgate.astype(jnp.float32))
    return (gated.astype(jnp.bfloat16), memory_next, norm_next, max_next)

def expert_apply(picked_rows, gate_matrix, up_matrix, down_matrix):
    gate_sums = jnp.dot(picked_rows, gate_matrix, preferred_element_type=jnp.float32)
    up_sums = jnp.dot(picked_rows, up_matrix, preferred_element_type=jnp.float32)
    hidden = (jax.nn.silu(gate_sums) * up_sums).astype(jnp.bfloat16)
    return jnp.dot(hidden, down_matrix, preferred_element_type=jnp.float32).astype(jnp.bfloat16)

def reference(tokens, first_gain, query_weight, key_weight, value_weight, outgate_weight, igate_weight, fgate_weight, igate_bias, fgate_bias, memory_state, norm_state, max_state, head_gain, out_weight, second_gain, expert_ids, route_weight, expert_gate, expert_up, expert_down, shared_gate, shared_up, shared_down):
    inputs = tokens.astype(jnp.float32)
    normed = rms_scale(inputs, first_gain).astype(jnp.bfloat16)
    query = jnp.dot(normed, query_weight, preferred_element_type=jnp.float32).astype(jnp.bfloat16)
    key_proj = jnp.dot(normed, key_weight, preferred_element_type=jnp.float32).astype(jnp.bfloat16)
    value_proj = jnp.dot(normed, value_weight, preferred_element_type=jnp.float32).astype(jnp.bfloat16)
    outgate = jnp.dot(normed, outgate_weight, preferred_element_type=jnp.float32).astype(jnp.bfloat16)
    gated, memory_next, norm_next, max_next = cell_step(normed, query, key_proj, value_proj, outgate, igate_weight, fgate_weight, igate_bias, fgate_bias, memory_state, norm_state, max_state, head_gain)
    mix = jnp.dot(gated, out_weight, preferred_element_type=jnp.float32).astype(jnp.bfloat16)
    stream = inputs + mix.astype(jnp.float32)
    normed_two = rms_scale(stream, second_gain).astype(jnp.bfloat16)
    padded = jnp.concatenate([normed_two, jnp.zeros((1, D), normed_two.dtype)], axis=0)

    def per_expert(routed, inputs_expert):
        expert_index, gate_matrix, up_matrix, down_matrix = inputs_expert
        chosen = expert_ids == expert_index
        weight = lax.optimization_barrier(jnp.sum(jnp.where(chosen, route_weight, jnp.zeros_like(route_weight)), axis=1))
        weight_pad = jnp.concatenate([weight, jnp.zeros((1,), weight.dtype)], axis=0)
        picked = jnp.nonzero(jnp.any(chosen, axis=1), size=N_EP * CAP, fill_value=SEQS)[0].astype(jnp.int32)
        result = expert_apply(padded[picked], gate_matrix, up_matrix, down_matrix)
        routed = routed.at[picked].add(weight_pad[picked][:, None] * result.astype(routed.dtype), mode='drop')
        return (routed, None)
    routed, _ = lax.scan(per_expert, jnp.zeros((SEQS, D), jnp.float32), (jnp.arange(EXPERTS, dtype=jnp.int32), expert_gate, expert_up, expert_down))
    gate_shared = jnp.dot(normed_two, shared_gate, preferred_element_type=jnp.float32)
    up_shared = jnp.dot(normed_two, shared_up, preferred_element_type=jnp.float32)
    hidden_shared = (jax.nn.silu(gate_shared) * up_shared).astype(jnp.bfloat16)
    shared_result = jnp.dot(hidden_shared, shared_down, preferred_element_type=jnp.float32)
    mixed_out = (stream + routed + shared_result).astype(jnp.bfloat16)
    return (mixed_out, memory_next, norm_next, max_next)
```

```python
import jax
import jax.numpy as jnp
from jax import lax
from jax.sharding import PartitionSpec as P

epsilon = 1e-06


def rms_scale(values, gain):
    return (
        values
        * lax.rsqrt(jnp.mean(values * values, axis=-1, keepdims=True) + epsilon)
        * gain.astype(jnp.float32)
    )


def cell_step(
    query,
    key_proj,
    value_proj,
    outgate,
    decay_rate,
    injected,
    max_next,
    memory_state,
    norm_state,
    head_gain,
):
    row_count, head_count = max_next.shape
    head_size = memory_state.shape[-1]
    query_heads = query.astype(jnp.float32).reshape(row_count, head_count, head_size)
    key_heads = key_proj.astype(jnp.float32).reshape(
        row_count, head_count, head_size
    ) * head_size ** (-0.5)
    value_heads = value_proj.astype(jnp.float32).reshape(row_count, head_count, head_size)
    memory_next = decay_rate[:, :, None, None] * memory_state + injected[:, :, None, None] * (
        key_heads[:, :, :, None] * value_heads[:, :, None, :]
    )
    norm_next = decay_rate[:, :, None] * norm_state + injected[:, :, None] * key_heads
    numerator = jnp.sum(query_heads[:, :, :, None] * memory_next, axis=2)
    denominator = jnp.maximum(
        jnp.abs(jnp.sum(query_heads * norm_next, axis=-1)), jnp.exp(-max_next)
    )
    readout = numerator / denominator[:, :, None]
    readout = rms_scale(readout, head_gain.reshape(head_count, head_size))
    gated = readout.reshape(row_count, head_count * head_size) * jax.nn.sigmoid(
        outgate.astype(jnp.float32)
    )
    return (gated.astype(jnp.bfloat16), memory_next, norm_next)


def shards(
    tokens,
    first_gain,
    query_weight,
    key_weight,
    value_weight,
    outgate_weight,
    igate_weight,
    fgate_weight,
    igate_bias,
    fgate_bias,
    memory_state,
    norm_state,
    max_state,
    head_gain,
    out_weight,
    second_gain,
    expert_ids,
    route_weight,
    expert_gate,
    expert_up,
    expert_down,
    shared_gate,
    shared_up,
    shared_down,
):
    rows, width = tokens.shape
    devices = lax.axis_size("ep")
    chips = devices // 2
    me = lax.axis_index("ep")
    chip, core = me // 2, me % 2
    groups = [[2 * j + c for j in range(chips)] for c in range(2)]
    partners = [(i, i ^ 1) for i in range(devices)]

    def swap(value):
        return lax.ppermute(value, "ep", partners)

    def exchange(blocks):
        return lax.all_to_all(
            blocks, "ep", split_axis=0, concat_axis=0, axis_index_groups=groups, tiled=True
        )

    def spread(block):
        return exchange(jnp.broadcast_to(block[None], (chips,) + block.shape))

    def paired(own, other, axis):
        return jnp.where(
            core == 0,
            jnp.concatenate([own, other], axis=axis),
            jnp.concatenate([other, own], axis=axis),
        )

    inputs = tokens.astype(jnp.float32)
    chosen = expert_ids[:, :, None] == jnp.arange(devices, dtype=jnp.int32)[None, None, :]
    dense = jnp.sum(jnp.where(chosen, route_weight[:, :, None], 0.0), axis=1)
    high = lax.reduce_precision(dense, 8, 7)
    extra = jnp.concatenate([high, dense - high], axis=1).astype(jnp.bfloat16)
    extra = jnp.pad(extra, ((0, 0), (0, -extra.shape[1] % 128)))
    gathered = spread(jnp.concatenate([tokens, extra], axis=1))
    gathered = gathered.reshape(chips * rows, -1)
    all_tokens = gathered[:, :width].astype(jnp.float32)
    routes = (
        gathered[:, width : width + devices].astype(jnp.float32)
        + gathered[:, width + devices : width + 2 * devices].astype(jnp.float32)
    )

    own_columns = jnp.stack([query_weight, key_weight, value_weight, outgate_weight], axis=1)
    other_columns = swap(own_columns)
    columns = paired(own_columns, other_columns, 2)
    chip_columns = columns.shape[2]
    columns = columns.reshape(width, 4 * chip_columns)

    normed_own = rms_scale(inputs, first_gain).astype(jnp.bfloat16)
    input_gate = jnp.dot(normed_own, igate_weight, preferred_element_type=jnp.float32) + igate_bias
    forget_log = jax.nn.log_sigmoid(
        jnp.dot(normed_own, fgate_weight, preferred_element_type=jnp.float32) + fgate_bias
    )
    max_next = jnp.maximum(forget_log + max_state, input_gate)
    decay_rate = jnp.exp(forget_log + max_state - max_next)
    injected = jnp.exp(input_gate - max_next)

    normed = rms_scale(all_tokens, first_gain).astype(jnp.bfloat16)
    projected = jnp.dot(normed, columns, preferred_element_type=jnp.float32).astype(jnp.bfloat16)
    arrived = exchange(projected.reshape(chips, rows, 4 * chip_columns))
    arrived = arrived.reshape(chips, rows, 4, chip_columns).transpose(2, 1, 0, 3)
    arrived = arrived.reshape(4, rows, chips * chip_columns)

    expert_own = (expert_gate[0], expert_up[0], expert_down[0])
    expert_other = tuple(swap(matrix) for matrix in expert_own)
    units = shared_gate.shape[1] // chips
    out_blocks = out_weight.reshape(-1, chips, width // chips).transpose(1, 0, 2)
    gate_blocks = jnp.concatenate(
        [
            matrix.reshape(-1, chips, units).transpose(1, 2, 0)
            for matrix in (shared_gate, shared_up)
        ],
        axis=2,
    )
    down_blocks = shared_down.reshape(chips, 2, units // 2, -1)
    down_blocks = jnp.concatenate([down_blocks[:, 0], down_blocks[:, 1]], axis=2)
    blocks = jnp.concatenate([out_blocks, gate_blocks, down_blocks], axis=1)
    blocks, arrived = lax.optimization_barrier((blocks, arrived))
    own_blocks = exchange(blocks)

    gated, memory_next, norm_next = cell_step(
        arrived[0],
        arrived[1],
        arrived[2],
        arrived[3],
        decay_rate,
        injected,
        max_next,
        memory_state,
        norm_state,
        head_gain,
    )
    all_gated = spread(gated).reshape(chips * rows, -1)

    other_blocks = swap(own_blocks)
    out_rows = out_weight.shape[0]
    out_columns = paired(own_blocks[:, :out_rows], other_blocks[:, :out_rows], 1)
    out_columns = out_columns.reshape(-1, width // chips)
    half = width // devices

    def shared_rows(lower, upper, part):
        own, other = (
            value[:, lower:upper, part * half : (part + 1) * half]
            for value in (own_blocks, other_blocks)
        )
        return paired(own, other, 2).transpose(1, 0, 2).reshape(upper - lower, width)

    shared_gate_rows = shared_rows(out_rows, out_rows + units, 0)
    shared_up_rows = shared_rows(out_rows, out_rows + units, 1)
    down_start = out_rows + units
    shared_down_rows = jnp.concatenate(
        [shared_rows(down_start, down_start + units // 2, part) for part in range(2)], axis=0
    )

    mix_columns = jnp.dot(all_gated, out_columns, preferred_element_type=jnp.float32).astype(
        jnp.bfloat16
    )
    mix = spread(mix_columns).transpose(1, 0, 2).reshape(chips * rows, width)
    stream = all_tokens + mix.astype(jnp.float32)
    normed_two = rms_scale(stream, second_gain).astype(jnp.bfloat16)

    total = jnp.zeros((chips * rows, width), jnp.float32)
    for (gate, up, down), index in ((expert_own, me), (expert_other, me ^ 1)):
        gate_sums = jnp.dot(normed_two, gate, preferred_element_type=jnp.float32)
        up_sums = jnp.dot(normed_two, up, preferred_element_type=jnp.float32)
        hidden = (jax.nn.silu(gate_sums) * up_sums).astype(jnp.bfloat16)
        result = jnp.dot(hidden, down, preferred_element_type=jnp.float32)
        total = total + lax.dynamic_slice_in_dim(routes, index, 1, 1) * result
    across = (((1,), (1,)), ((), ()))
    gate_sums = lax.dot_general(
        normed_two, shared_gate_rows, across, preferred_element_type=jnp.float32
    )
    up_sums = lax.dot_general(
        normed_two, shared_up_rows, across, preferred_element_type=jnp.float32
    )
    hidden = (jax.nn.silu(gate_sums) * up_sums).astype(jnp.bfloat16)
    total = total + jnp.dot(hidden, shared_down_rows, preferred_element_type=jnp.float32)

    returned = exchange(total.astype(jnp.bfloat16).reshape(chips, rows, width))
    own_stream = lax.dynamic_slice_in_dim(stream, chip * rows, rows, 0)
    mixed_out = own_stream + jnp.sum(returned.astype(jnp.float32), axis=0)
    return (mixed_out.astype(jnp.bfloat16), memory_next, norm_next, max_next)


def solution(mesh):
    placed = (
        P(("grp", "ep"), None),
        P(),
        P(None, "ep"),
        P(None, "ep"),
        P(None, "ep"),
        P(None, "ep"),
        P(),
        P(),
        P(),
        P(),
        P(("grp", "ep"), None, None, None),
        P(("grp", "ep"), None, None),
        P(("grp", "ep"), None),
        P(),
        P("ep", None),
        P(),
        P(("grp", "ep"), None),
        P(("grp", "ep"), None),
        P("ep", None, None),
        P("ep", None, None),
        P("ep", None, None),
        P("ep", None),
        P("ep", None),
        P(None, "ep"),
    )
    return jax.shard_map(
        shards,
        mesh=mesh,
        in_specs=placed,
        out_specs=(
            P(("grp", "ep"), None),
            P(("grp", "ep"), None, None, None),
            P(("grp", "ep"), None, None),
            P(("grp", "ep"), None),
        ),
        check_vma=False,
    )
```
